1024 devices in a mesh: rep: 4 (over z_hi), fs: 32 (over z_lo, y), tp: 8 (over x, core).
Axes of the slice: x: 4, y: 4, z: 32 (z_hi: 4, z_lo: 8; z = z_hi * 8 + z_lo), core: 2. Of those that a mesh axis runs over, the one named last changes fastest.
Arguments:
- residual: bfloat16 [128, 256, 2048], P(('rep', 'fs'), None, 'tp'), may hold values from -6 to 6
- queries: bfloat16 [128, 256, 2048], P(('rep', 'fs'), None, 'tp'), may hold values from -6 to 6
- key_matrix: bfloat16 [128, 256, 2048], P(('rep', 'fs'), None, 'tp'), may hold values from -6 to 6
- value_matrix: bfloat16 [128, 256, 2048], P(('rep', 'fs'), None, 'tp'), may hold values from -6 to 6
- decay_logodds: float32 [128, 256, 2048], P(('rep', 'fs'), None, 'tp'), may hold values from -3.4 to 8.9, as said below
- decay_surge: float32 [128, 256, 8], P(('rep', 'fs'), None, 'tp'), may hold values from -2.1 to 0, as said below
- head_norm_gain: float32 [256], replicated, may hold values from 0.1 to 1.9
- output_matrix: float32 [2048, 2048], P('fs', 'tp'), may hold values from -0.125 to 0.125
- output_column_scale: float32 [2048], P('tp'), may hold values from 0.5 to 2
- premix_norm_gain: float32 [2048], replicated, may hold values from 0.1 to 1.9
- gate_matrix: float32 [2048, 2816], P('fs', 'tp'), may hold values from -0.125 to 0.125
- gate_column_scale: float32 [2816], P('tp'), may hold values from 0.5 to 2
- up_matrix: float32 [2048, 2816], P('fs', 'tp'), may hold values from -0.125 to 0.125
- up_column_scale: float32 [2816], P('tp'), may hold values from 0.5 to 2
- down_matrix: float32 [2048, 2816], P('fs', 'tp'), may hold values from -0.109375 to 0.109375
- down_column_scale: float32 [2048], P('tp'), may hold values from 0.5 to 2
Outputs:
- layer_out: bfloat16 [128, 256, 2048], P(('rep', 'fs'), None, 'tp')
The draws below stay inside these ranges and needn't reach their ends.
Inputs may be any that keep to these rules, and one draw needn't show every extreme that they name: `decay_logodds`: log-odds of a key channel's decay. `decay_surge`: non-positive log-factors of a head's state.
All inputs are finite; a program needn't handle non-finite values.
Results may differ from the reference program's by a relative error of at most 0.018.
Values may be sent and summed in bfloat16 or wider, within the bound.
A program may use at most 32 MiB of HBM per device.

```python
import math
import jax
import jax.numpy as jnp
from jax import lax

D = 2048
HEAD_NUMBER = 8
HEAD_V = 256
FF = 2816
BLOCK = 64
SEQUENCE_LENGTH = 256
KEY_DIM = 2048
VALUE_DIM = 2048
BATCH_SIZE = 128
N_TP = 8


def draw_decay_logodds(key, part):
    residual_flows = jax.random.split(jax.random.fold_in(key, 11), 5)
    slow_share = 0.5
    jitter = jnp.clip(0.7 * jax.random.normal(residual_flows[4], (BATCH_SIZE, SEQUENCE_LENGTH, KEY_DIM), jnp.float32), -2.8, 2.8)
    slow_mask = jax.random.uniform(residual_flows[0], (KEY_DIM,), jnp.float32) < slow_share
    slow_base = jax.random.uniform(residual_flows[1], (KEY_DIM,), jnp.float32, 3.5, 5.5)
    fast_base = jax.random.uniform(residual_flows[2], (KEY_DIM,), jnp.float32, 0.0, 1.2)
    offset = jax.random.uniform(residual_flows[3], (BATCH_SIZE, 1, 1), jnp.float32, -0.6, 0.6)
    return jnp.where(slow_mask, slow_base, fast_base) + offset + jitter


def draw_decay_surge(key, part):
    residual_flows = jax.random.split(jax.random.fold_in(key, 23), 2)
    surge_position = jax.random.randint(residual_flows[0], (BATCH_SIZE, 3, HEAD_NUMBER), 0, SEQUENCE_LENGTH)
    strength = jnp.log(jax.random.uniform(residual_flows[1], (BATCH_SIZE, 3, HEAD_NUMBER), jnp.float32, 0.5, 0.8))
    match_scores = jnp.arange(SEQUENCE_LENGTH)[None, :, None, None] == surge_position[:, None, :, :]
    return jnp.sum(jnp.where(match_scores, strength[:, None, :, :], 0.0), axis=2)


def block_levels(own_key, shape, cuts, low, top_value):
    def one(position, shards_of):
        draws = jax.random.uniform(jax.random.fold_in(jax.random.fold_in(own_key, 6), position), (shards_of,), jnp.float32, low / len(cuts), top_value / len(cuts))
        return jnp.repeat(jnp.exp(draws), shape[position] // shards_of).reshape((-1,) + (1,) * (len(shape) - position - 1))

    loudness = one(*cuts[0])
    for cut in cuts[1:]:
        loudness = loudness * one(*cut)
    return loudness


def gaussian(stream_key, dims, scale, bound, cuts=(), kind=jnp.bfloat16):
    values = jax.random.normal(stream_key, dims, jnp.float32) * scale
    if len(cuts) > 0:
        values = block_levels(stream_key, dims, cuts, -0.22, 0.18) * values
    return jnp.clip(values, min=-bound, max=bound).astype(kind)


def setup_inputs(seed: int = 0) -> dict:
    arg_keys = jax.random.split(jax.random.key(seed), 17)
    return {
        "residual": gaussian(arg_keys[0], (BATCH_SIZE, SEQUENCE_LENGTH, D), 1.0, 6.0, ((0, 128), (2, 8))),
        "queries": gaussian(arg_keys[1], (BATCH_SIZE, SEQUENCE_LENGTH, KEY_DIM), 1.0, 6.0, ((0, 128), (2, 8))),
        "key_matrix": gaussian(arg_keys[2], (BATCH_SIZE, SEQUENCE_LENGTH, KEY_DIM), 1.0, 6.0, ((0, 128), (2, 8))),
        "value_matrix": gaussian(arg_keys[3], (BATCH_SIZE, SEQUENCE_LENGTH, VALUE_DIM), 1.0, 6.0, ((0, 128), (2, 8))),
        "decay_logodds": draw_decay_logodds(jax.random.fold_in(arg_keys[16], 71), 0),
        "decay_surge": draw_decay_surge(jax.random.fold_in(arg_keys[16], 71), 0),
        "head_norm_gain": jnp.clip(1.0 + 0.18 * jax.random.normal(arg_keys[6], (HEAD_V,), jnp.float32), 0.1, 1.9),
        "output_matrix": gaussian(arg_keys[7], (D, VALUE_DIM), VALUE_DIM ** -0.5, 0.125, ((0, 32), (1, 8)), jnp.float32),
        "output_column_scale": jnp.clip(jnp.exp(math.log(2.0) - 1.3862944 * jax.random.uniform(arg_keys[8], (D,), jnp.float32) ** block_levels(arg_keys[8], (D,), ((0, 8),), -0.2, 0.2)), 0.5, 2.0),
        "premix_norm_gain": jnp.clip(1.0 + 0.18 * jax.random.normal(arg_keys[9], (D,), jnp.float32), 0.1, 1.9),
        "gate_matrix": gaussian(arg_keys[10], (D, FF), D ** -0.5, 0.125, ((0, 32), (1, 8)), jnp.float32),
        "gate_column_scale": jnp.clip(jnp.exp(math.log(2.0) - 1.3862944 * jax.random.uniform(arg_keys[11], (FF,), jnp.float32) ** block_levels(arg_keys[11], (FF,), ((0, 8),), -0.2, 0.2)), 0.5, 2.0),
        "up_matrix": gaussian(arg_keys[12], (D, FF), D ** -0.5, 0.125, ((0, 32), (1, 8)), jnp.float32),
        "up_column_scale": jnp.clip(jnp.exp(math.log(2.0) - 1.3862944 * jax.random.uniform(arg_keys[13], (FF,), jnp.float32) ** block_levels(arg_keys[13], (FF,), ((0, 8),), -0.2, 0.2)), 0.5, 2.0),
        "down_matrix": gaussian(arg_keys[14], (D, FF), FF ** -0.5, 0.109375, ((0, 32), (1, 8)), jnp.float32),
        "down_column_scale": jnp.clip(jnp.exp(math.log(2.0) - 1.3862944 * jax.random.uniform(arg_keys[15], (D,), jnp.float32) ** block_levels(arg_keys[15], (D,), ((0, 8),), -0.2, 0.2)), 0.5, 2.0),
    }


epsilon = 1e-06
softness_factor = 16.0
highest = lax.Precision.HIGHEST

def one_direction(query_heads, key_heads, value_heads, log_decay_values):
    sequence_batch, head_total, token_length, key_channel_width = query_heads.shape
    value_width = value_heads.shape[-1]
    block_count = token_length // BLOCK

    def blocks(tensor):
        return tensor.reshape(sequence_batch, head_total, block_count, BLOCK, tensor.shape[-1])
    q_blocks = blocks(query_heads)
    k_blocks = blocks(key_heads)
    v_blocks = blocks(value_heads)
    running = jnp.cumsum(blocks(log_decay_values), axis=3)
    block_end = running[:, :, :, -1:, :]
    q_dec = q_blocks * jnp.exp(running)
    k_inv = k_blocks * jnp.exp(-running)
    k_end = k_blocks * jnp.exp(block_end - running)
    lower_mask = jnp.tril(jnp.ones((BLOCK, BLOCK), jnp.float32))
    scores = jnp.einsum('shnid,shnjd->shnij', q_dec, k_inv, precision=highest) * lower_mask
    inner_part = jnp.einsum('shnij,shnje->shnie', scores, v_blocks, precision=highest)
    fading = jnp.exp(block_end[:, :, :, 0, :])

    def advance(memory, pieces):
        q_piece, k_piece, v_piece, f_piece = pieces
        carried = jnp.einsum('shcd,shde->shce', q_piece, memory, precision=highest)
        memory = f_piece[..., None] * memory + jnp.einsum('shcd,shce->shde', k_piece, v_piece, precision=highest)
        return (memory, carried)
    pieces = tuple((jnp.moveaxis(tensor, 2, 0) for tensor in (q_dec, k_end, v_blocks, fading)))
    initial = jnp.zeros((sequence_batch, head_total, key_channel_width, value_width), jnp.float32)
    _, carried = lax.scan(advance, initial, pieces)
    summed = inner_part + jnp.moveaxis(carried, 0, 2)
    return summed.reshape(sequence_batch, head_total, token_length, value_width)

def backwards(tensor):
    return tensor[:, :, ::-1]

def linear_attend(queries, key_matrix, value_matrix, decay_logodds, decay_surge, head_norm_gain):
    sequence_batch, token_length, head_total = decay_surge.shape
    key_channel_width = queries.shape[-1] // head_total
    value_width = value_matrix.shape[-1] // head_total

    def split_heads(tensor, width):
        return jnp.transpose(tensor.astype(jnp.float32).reshape(sequence_batch, token_length, head_total, width), (0, 2, 1, 3))
    query_heads = split_heads(queries, key_channel_width) * key_channel_width ** (-0.5)
    key_heads = split_heads(key_matrix, key_channel_width)
    value_heads = split_heads(value_matrix, value_width)
    gate_values = jax.nn.log_sigmoid(decay_logodds).reshape(sequence_batch, token_length, head_total, key_channel_width) / softness_factor
    log_decay_values = jnp.transpose(gate_values + decay_surge[..., None], (0, 2, 1, 3))
    forward = one_direction(query_heads, key_heads, value_heads, log_decay_values)
    backward = backwards(one_direction(backwards(query_heads), backwards(key_heads), backwards(value_heads), backwards(log_decay_values)))
    attended = forward + backward
    scaled = attended * lax.rsqrt(lax.optimization_barrier(jnp.mean(attended * attended, axis=-1, keepdims=True)) + epsilon) * head_norm_gain
    merged = jnp.transpose(scaled, (0, 2, 1, 3)).reshape(sequence_batch * token_length, head_total * value_width)
    return merged.astype(jnp.bfloat16)

def grouped(left, right):
    width = left.shape[1] // N_TP
    left_parts = left.reshape(left.shape[0], N_TP, width).astype(jnp.float32)
    right_parts = right.reshape(right.shape[0], N_TP, width).astype(jnp.float32)
    terms = jnp.einsum('lgc,dgc->gld', left_parts, right_parts, precision=highest)
    rounded = lax.optimization_barrier(terms.astype(jnp.bfloat16))
    return lax.optimization_barrier(jnp.sum(rounded.astype(jnp.float32), axis=0))

def rms_scaled(rows_in, gain):
    wide_rows = rows_in.astype(jnp.float32)
    factor = lax.rsqrt(lax.optimization_barrier(jnp.mean(wide_rows * wide_rows, axis=-1, keepdims=True)) + epsilon)
    return (wide_rows * factor * gain).astype(jnp.bfloat16)

def reference(residual, queries, key_matrix, value_matrix, decay_logodds, decay_surge, head_norm_gain, output_matrix, output_column_scale, premix_norm_gain, gate_matrix, gate_column_scale, up_matrix, up_column_scale, down_matrix, down_column_scale):
    out_half = output_matrix.astype(jnp.bfloat16)
    gate_half = gate_matrix.astype(jnp.bfloat16)
    up_half = up_matrix.astype(jnp.bfloat16)
    down_half = down_matrix.astype(jnp.bfloat16)

    def single_sequence(input_rows):
        residual_sequence, query_sequence, key_sequence, value_sequence, logodds_sequence, surge_sequence = input_rows
        normalized_rows = linear_attend(query_sequence[None], key_sequence[None], value_sequence[None], logodds_sequence[None], surge_sequence[None], head_norm_gain)
        mix_total = grouped(normalized_rows, out_half)
        updated = (residual_sequence.astype(jnp.float32) + output_column_scale * mix_total).astype(jnp.bfloat16)
        normin = rms_scaled(updated, premix_norm_gain)
        gate_pre = jnp.dot(normin, gate_half, preferred_element_type=jnp.float32) * gate_column_scale
        up_pre = jnp.dot(normin, up_half, preferred_element_type=jnp.float32) * up_column_scale
        hidden = (jax.nn.silu(gate_pre) * up_pre).astype(jnp.bfloat16)
        down_total = grouped(hidden, down_half)
        return (updated.astype(jnp.float32) + down_column_scale * down_total).astype(jnp.bfloat16)
    return lax.map(single_sequence, (residual, queries, key_matrix, value_matrix, decay_logodds, decay_surge))
```

```python
import functools

import jax
import jax.numpy as jnp
from jax import lax
from jax.experimental import pallas as pl
from jax.experimental.pallas import tpu as pltpu
from jax.sharding import PartitionSpec as P

MESH = pl.DeviceIdType.MESH
F32, BF16 = jnp.float32, jnp.bfloat16
EPS = 1e-06

RELAY_Z = [(0, 1, 0), (0, -1, 0), (1, 2, 0), (-1, -2, 0), (2, 3, 0), (-2, -3, 0), (3, 4, 1), (-3, -4, 2)]
DIRECT_Z = [(0, 1, 0), (0, -1, 0), (0, 2, 0), (0, -2, 0), (0, 3, 0), (0, -3, 0), (0, 4, 1), (0, -4, 2)]
SKIP_Z = [(0, 1, 0), (0, -1, 0), (0, 2, 0), (0, -2, 0), (2, 3, 0), (-2, -3, 0), (2, 4, 1), (-2, -4, 2)]
RELAY_Y = [(0, 1, 0), (0, -1, 0), (1, 2, 1), (-1, -2, 2)]
DIRECT_Y = [(0, 1, 0), (0, -1, 0), (0, 2, 1), (0, -2, 2)]
OFFSETS = (0, 1, -1, 2, -2, 3, -3, 4)

STAGES = ((16, SKIP_Z, DIRECT_Y), (32, RELAY_Z, RELAY_Y), (16, RELAY_Z, RELAY_Y))
HALVES = 2
N_GATHER = 52
N_REDUCE = 7 * HALVES
N_SPREAD = 7 * HALVES
N_COPIES = 3 * N_GATHER + 2 * N_REDUCE + N_SPREAD

ORDER = (
    ("A0", "B0", "C0", "pre", "att0", "att1", "att2", "att3", "A1", "A2", "B1", "C1", "A9"),
    ("R0", "B2", "C2", "R1", "B3", "C3", "R2", "B4", "C4", "S0", "B5", "C5", "S1", "B6", "C6", "S2", "B9"),
    ("H0", "C9", "D0", "D1", "D2", "O0"),
)


def dot_rows(a, b):
    return lax.dot_general(a, b, (((1,), (1,)), ((), ())), preferred_element_type=F32)


def dot_plain(a, b):
    return lax.dot_general(a, b, (((1,), (0,)), ((), ())), preferred_element_type=F32)


def kernel(*refs):
    inputs, rest = refs[:16], refs[16:]
    upd_ref, tot_ref = rest[:2]
    staged, rest = rest[2:18], rest[18:]
    (
        wa, wb, wc, lc, mc, nrm, hid, uall, nin,
        px, pr, own, sa, sb, sc, ra, rb, rc,
        load_sem, send_sem, recv_sem,
    ) = rest
    res, q, k, v, lod, sur, hg, ow, ocs, png, gw, gcs, uw, ucs, dw, dcs = staged
    rep, fs, tp = (lax.axis_index(n) for n in ("rep", "fs", "tp"))
    zl, y = lax.div(fs, 4), lax.rem(fs, 4)
    x, c = lax.div(tp, 2), lax.rem(tp, 2)
    z = rep * 8 + zl
    sgn = 1 - 2 * c

    def at(dz=0, dy=0):
        zz = lax.rem(z + dz + 32, 32)
        return (lax.div(zz, 8), lax.rem(zz, 8) * 4 + lax.rem(y + dy + 4, 4), tp)

    def at_x(dx):
        return (rep, fs, 2 * lax.rem(x + dx + 4, 4) + c)

    partner = (rep, fs, 2 * x + 1 - c)

    class Copy:
        def __init__(self, i):
            self.i, self.sent, self.got = i, None, False

        def start(self, src, dst, to):
            self.sent = pltpu.make_async_remote_copy(
                src_ref=src, dst_ref=dst, send_sem=send_sem.at[self.i], recv_sem=recv_sem.at[self.i],
                device_id=to, device_id_type=MESH)
            self.sent.start()

        def wait(self, dst, to):
            if not self.got:
                self.got = True
                pltpu.make_async_remote_copy(
                    src_ref=dst, dst_ref=dst, send_sem=send_sem.at[self.i], recv_sem=recv_sem.at[self.i],
                    device_id=to, device_id_type=MESH).wait_recv()

    copies = [Copy(i) for i in range(N_COPIES)]
    free = iter(copies)

    barrier = pltpu.get_barrier_semaphore()
    peers = []
    dzs = sorted({child - parent for _, tree, _ in STAGES for parent, child, _ in tree})
    dys = sorted({child - parent for _, _, tree in STAGES for parent, child, _ in tree} - {-2})
    peers += [at(dz=d) for d in dzs] + [at(dy=d) for d in dys] + [at_x(1), at_x(-1), partner]
    for peer in peers:
        pl.semaphore_signal(barrier, inc=1, device_id=peer, device_id_type=MESH)

    loads = [pltpu.make_async_copy(inputs[i], staged[i], load_sem.at[i]) for i in range(16)]
    for i in (7, 10, 12, 14, 4, 5, 1, 2, 3, 6, 0, 8, 9, 11, 13, 15):
        loads[i].start()
    for i in (7, 10, 12, 14):
        loads[i].wait()
    wa[zl, y] = ow[...].astype(BF16)
    zpad = jnp.zeros((64, 32), BF16)
    wb[zl, y, :, 0:352] = gw[...].astype(BF16)
    wb[zl, y, :, 352:384] = zpad
    wb[zl, y, :, 384:736] = uw[...].astype(BF16)
    wb[zl, y, :, 736:768] = zpad
    wc[zl, y, :, 0:352] = dw[...].astype(BF16)
    wc[zl, y, :, 352:384] = zpad
    pl.semaphore_wait(barrier, len(peers))

    def stage_steps(buf, p, ztree, ytree):
        cp = {}

        def plane(d):
            return lax.rem(zl - d + 8, 8)

        def q_slice(dz, dy, part):
            zz, yy = plane(dz), lax.rem(y - dy + 4, 4)
            return zz, yy

        def q_ref(dz, dy, zpart, ypart):
            rows = 64 - p
            cut = 16 * (rows // 32) if rows > 16 else 0
            lo, hi = p, 64
            for part in (zpart, ypart):
                if part == 1:
                    hi = p + cut
                if part == 2:
                    lo = p + cut
            return buf.at[plane(dz), lax.rem(y - dy + 4, 4), lo:hi]

        def p_ref(dy, part):
            lo, hi = (0, p)
            if p > 16:
                if part == 1:
                    hi = p // 2
                if part == 2:
                    lo = p // 2
            return buf.at[zl, lax.rem(y - dy + 4, 4), lo:hi]

        def b_ref(dz, part):
            lo, hi = (0, 4) if part == 0 else ((0, 2) if part == 1 else (2, 4))
            return buf.at[plane(dz), lo:hi, 0:p]

        def p_skip(part):
            return p <= 16 and part == 2

        table = {}
        for parent, child, part in ytree:
            if p and not p_skip(part):
                table["py", child] = (parent, part)
        for parent, child, part in ztree:
            if p:
                table["pz", child] = (parent, part)
            table["qz", child] = (parent, part)
        for d in OFFSETS:
            for parent, child, part in ytree:
                table["qy", d, child] = (parent, part)
        for key in table:
            cp[key] = next(free)

        def refs(key, back):
            parent, part = table[key]
            d = parent if back else key[-1]
            step = key[-1] - parent
            if key[0] == "py":
                return p_ref(d, part), at(dy=step)
            if key[0] == "pz":
                return b_ref(d, part), at(dz=step)
            if key[0] == "qz":
                return q_ref(d, 0, part, 0), at(dz=step)
            return q_ref(key[1], d, 0, part), at(dy=step)

        def send(key):
            if key not in table:
                return
            parent = table[key][0]
            if key[0] in ("py", "qz"):
                if parent:
                    wait(key[:-1] + (parent,))
            elif key[0] == "pz":
                if parent:
                    wait(("pz", parent))
                else:
                    for n in (1, -1, 2, -2):
                        wait(("py", n))
            else:
                if parent:
                    wait(key[:-1] + (parent,))
                elif key[1] == 4:
                    wait(("qz", 4))
                    wait(("qz", -4))
                elif key[1]:
                    wait(("qz", key[1]))
            src, to = refs(key, True)
            cp[key].start(src, src, to)

        def wait(key):
            if key in table:
                dst, to = refs(key, False)
                cp[key].wait(dst, to)

        depth = {0: 0}
        for parent, child, _ in ztree:
            depth[child] = depth[parent] + 1
        last = max(depth.values())
        steps = []

        def add(r, key):
            while len(steps) <= r:
                steps.append([])
            steps[r].append(key)

        for key in [("py", 1), ("py", -1)]:
            add(0, key)
        ydepth = {0: 0}
        for parent, child, _ in ytree:
            ydepth[child] = ydepth[parent] + 1
        for key in [("py", 2), ("py", -2)]:
            add(ydepth[2] - 1, key)
        for parent, child, _ in ztree:
            add(depth[child] - 1, ("qz", child))
            add(depth[child] - 1 + ydepth[2], ("pz", child))
        for d in OFFSETS:
            for child in (1, -1):
                add(depth[d], ("qy", d, child))
            for child in (2, -2):
                add(depth[d] + ydepth[2] - 1, ("qy", d, child))

        def run(r):
            if r < len(steps):
                for key in steps[r]:
                    send(key)
            if r == 9:
                for key in table:
                    wait(key)

        return run

    stage = {
        "A": stage_steps(wa, *STAGES[0]),
        "B": stage_steps(wb, *STAGES[1]),
        "C": stage_steps(wc, *STAGES[2]),
    }

    def pre():
        for i in (4, 5, 1, 2, 3, 6, 0, 8, 9, 11, 13, 15):
            loads[i].wait()
        u = lod[...]
        ls = -(jnp.maximum(-u, 0.0) + jnp.log1p(jnp.exp(-jnp.abs(u)))) * (1.0 / 16.0)
        row = lax.broadcasted_iota(jnp.int32, (256, 256), 0)
        col = lax.broadcasted_iota(jnp.int32, (256, 256), 1)
        tri = jnp.where(col <= row, 1.0, 0.0).astype(BF16)
        hi = ls.astype(BF16)
        r1 = ls - hi.astype(F32)
        mid = r1.astype(BF16)
        lo = (r1 - mid.astype(F32)).astype(BF16)
        total = dot_plain(tri, hi) + (dot_plain(tri, mid) + dot_plain(tri, lo))
        srow = jnp.broadcast_to(sur[...], (256, 256))
        upto = jnp.sum(jnp.where(col <= row, srow, 0.0), axis=1, keepdims=True)
        before = jnp.sum(jnp.where(col < row, srow, 0.0), axis=1, keepdims=True)
        lc[...] = total + upto
        mc[...] = (total - ls) + before

    def attend(i):
        a, b = 64 * i, 64 * i + 64
        li, mi = lc[a:b], mc[a:b]
        qi, ki = q[a:b].astype(F32), k[a:b].astype(F32)
        mid = lc[a + 31 : a + 32]
        sf = dot_rows((qi * jnp.exp(li - mid)).astype(BF16), (ki * jnp.exp(mid - li)).astype(BF16))
        sb_ = dot_rows((qi * jnp.exp(mid - mi)).astype(BF16), (ki * jnp.exp(mi - mid)).astype(BF16))
        row = lax.broadcasted_iota(jnp.int32, (64, 64), 0)
        col = lax.broadcasted_iota(jnp.int32, (64, 64), 1)
        s = jnp.where(col <= row, sf, 0.0) + jnp.where(col >= row, sb_, 0.0)
        o = dot_plain(s.astype(BF16), v[a:b])
        if i > 0:
            edge = lc[a - 1 : a]
            kf = (k[0:a].astype(F32) * jnp.exp(edge - lc[0:a])).astype(BF16)
            s = dot_rows((qi * jnp.exp(li - edge)).astype(BF16), kf)
            o += dot_plain(s.astype(BF16), v[0:a])
        if i < 3:
            edge = lc[b - 1 : b]
            kb = (k[b:256].astype(F32) * jnp.exp(mc[b:256] - edge)).astype(BF16)
            s = dot_rows((qi * jnp.exp(edge - mi)).astype(BF16), kb)
            o += dot_plain(s.astype(BF16), v[b:256])
        o = o * (1.0 / 16.0)
        ms = jnp.mean(o * o, axis=1, keepdims=True)
        nrm[a:b] = (o * lax.rsqrt(ms + EPS) * hg[...]).astype(BF16)

    def ring_x(r, s):
        return lax.rem(x + (2, 4 - s, 4 + s, 0)[r], 4)

    T = 256 // HALVES

    def reducer(idx, lhs, weights):
        cps = [[next(free) for _ in range(7)] for _ in range(HALVES)]

        def w(j):
            full = weights[j]
            return full.reshape(256, full.shape[-1])

        def rows(h):
            return slice(h * T, h * T + T)

        def first(h):
            cp = cps[h]
            for r in range(4):
                px[idx, h, r] = dot_rows(lhs[rows(h)], w(2 * ring_x(r, -sgn) + 1 - c)).astype(BF16)
            for r in range(4):
                own[h, r] = dot_rows(lhs[rows(h)], w(2 * ring_x(r, sgn) + c))
                cp[r].start(px.at[idx, h, r], pr.at[idx, h, r], partner)

        def second(h):
            cp = cps[h]
            for r, buf in ((0, sa), (1, sb)):
                cp[r].wait(pr.at[idx, h, r], partner)
                buf[idx, h] = (own[h, r] + pr[idx, h, r].astype(F32)).astype(BF16)
            for r in (2, 3):
                cp[r].wait(pr.at[idx, h, r], partner)
                own[h, r] = own[h, r] + pr[idx, h, r].astype(F32)
            cp[4].start(sa.at[idx, h], ra.at[idx, h], at_x(sgn))
            cp[5].start(sb.at[idx, h], rb.at[idx, h], at_x(-sgn))

        def third(h):
            cp = cps[h]
            cp[4].wait(ra.at[idx, h], at_x(sgn))
            sc[idx, h] = (own[h, 2] + ra[idx, h].astype(F32)).astype(BF16)
            cp[6].start(sc.at[idx, h], rc.at[idx, h], at_x(sgn))

        def total(h):
            cp = cps[h]
            cp[5].wait(rb.at[idx, h], at_x(-sgn))
            cp[6].wait(rc.at[idx, h], at_x(sgn))
            return own[h, 3] + rb[idx, h].astype(F32) + rc[idx, h].astype(F32)

        return first, second, third, total, rows

    mix = reducer(0, nrm, wa)
    down = reducer(1, hid, wc)

    cps = [[next(free) for _ in range(7)] for _ in range(HALVES)]

    def u_ref(h, j):
        return uall.at[j, h * T : h * T + T]

    def spread_own(h):
        cp = cps[h]
        total = mix[3](h)
        sl = mix[4](h)
        u = (res[sl].astype(F32) + ocs[...] * total).astype(BF16)
        uall[tp, sl] = u
        upd_ref[sl] = u
        cp[0].start(u_ref(h, tp), u_ref(h, tp), at_x(sgn))
        cp[1].start(u_ref(h, tp), u_ref(h, tp), at_x(-sgn))
        cp[3].start(u_ref(h, tp), u_ref(h, tp), partner)

    def spread_on(h):
        cp = cps[h]
        j = 2 * ring_x(1, sgn) + c
        cp[0].wait(u_ref(h, j), at_x(sgn))
        cp[2].start(u_ref(h, j), u_ref(h, j), at_x(sgn))
        cp[4].start(u_ref(h, j), u_ref(h, j), partner)
        j = 2 * ring_x(2, sgn) + c
        cp[1].wait(u_ref(h, j), at_x(-sgn))
        cp[5].start(u_ref(h, j), u_ref(h, j), partner)

    def spread_end(h):
        cp = cps[h]
        j = 2 * ring_x(0, sgn) + c
        cp[2].wait(u_ref(h, j), at_x(sgn))
        cp[6].start(u_ref(h, j), u_ref(h, j), partner)

    def normalise(h):
        cp = cps[h]
        for n, r in ((3, 3), (4, 1), (5, 2), (6, 0)):
            cp[n].wait(u_ref(h, 2 * ring_x(r, -sgn) + 1 - c), partner)
        sl = mix[4](h)
        ssq = jnp.zeros((T, 1), F32)
        for j in range(8):
            u = uall[j, sl].astype(F32)
            ssq += jnp.sum(u * u, axis=1, keepdims=True)
        factor = lax.rsqrt(ssq * (1.0 / 2048.0) + EPS)
        for j in range(8):
            u = uall[j, sl].astype(F32)
            nin[sl, 256 * j : 256 * j + 256] = (u * factor * png[:, 256 * j : 256 * j + 256]).astype(BF16)

    def hidden(h):
        normalise(h)
        sl = mix[4](h)
        gu = dot_plain(nin[sl], wb[...].reshape(2048, 768))
        g = gu[:, 0:352] * gcs[...]
        up = gu[:, 384:736] * ucs[...]
        hid[sl, 0:352] = (g / (1.0 + jnp.exp(-g)) * up).astype(BF16)
        hid[sl, 352:384] = jnp.zeros((T, 32), BF16)

    def out(h):
        sl = mix[4](h)
        tot_ref[sl] = dcs[...] * down[3](h)

    per_half = {
        "R0": mix[0], "R1": mix[1], "R2": mix[2], "S0": spread_own, "S1": spread_on, "S2": spread_end,
        "H0": hidden, "D0": down[0], "D1": down[1], "D2": down[2], "O0": out,
    }

    for token in sum(ORDER, ()):
        if token[0] in stage:
            stage[token[0]](int(token[1:]))
        elif token == "pre":
            pre()
        elif token[:3] == "att":
            attend(int(token[3:]))
        elif token[2:] == "":
            for h in range(HALVES):
                per_half[token](h)
        else:
            per_half[token[:2]](int(token[2:]))

    for cp in copies:
        if cp.sent is not None:
            cp.sent.wait_send()


def body(res, q, k, v, lod, sur, hg, ow, ocs, png, gw, gcs, uw, ucs, dw, dcs):
    rows = 256
    flat = (
        res.reshape(rows, -1), q.reshape(rows, -1), k.reshape(rows, -1), v.reshape(rows, -1),
        lod.reshape(rows, -1), sur.reshape(1, rows), hg.reshape(1, -1), ow, ocs.reshape(1, -1),
        png.reshape(1, -1), gw, gcs, uw, ucs, dw, dcs.reshape(1, -1),
    )
    H, T = HALVES, 256 // HALVES
    vm = pltpu.VMEM
    upd, total = pl.pallas_call(
        kernel,
        name="layer",
        out_shape=(jax.ShapeDtypeStruct((rows, 256), BF16), jax.ShapeDtypeStruct((rows, 256), F32)),
        in_specs=[pl.BlockSpec(memory_space=pl.ANY)] * 16,
        out_specs=[pl.BlockSpec(memory_space=pltpu.VMEM)] * 2,
        scratch_shapes=[vm(a.shape, a.dtype) for a in flat] + [
            vm((8, 4, 64, 256), BF16), vm((8, 4, 64, 768), BF16), vm((8, 4, 64, 384), BF16),
            vm((256, 256), F32), vm((256, 256), F32), vm((256, 256), BF16), vm((256, 384), BF16),
            vm((8, 256, 256), BF16), vm((256, 2048), BF16),
            vm((2, H, 4, T, 256), BF16), vm((2, H, 4, T, 256), BF16), vm((H, 4, T, 256), F32),
            vm((2, H, T, 256), BF16), vm((2, H, T, 256), BF16), vm((2, H, T, 256), BF16),
            vm((2, H, T, 256), BF16), vm((2, H, T, 256), BF16), vm((2, H, T, 256), BF16),
            pltpu.SemaphoreType.DMA((16,)),
            pltpu.SemaphoreType.DMA((N_COPIES,)), pltpu.SemaphoreType.DMA((N_COPIES,)),
        ],
        compiler_params=pltpu.CompilerParams(
            collective_id=0, has_side_effects=True, vmem_limit_bytes=56 * 2**20),
    )(*flat)
    result = (upd.astype(F32) + total).astype(BF16)
    return result.reshape(1, rows, 256)


def solution(mesh):
    seq = P(("rep", "fs"), None, "tp")
    return jax.shard_map(
        body,
        mesh=mesh,
        in_specs=(
            seq, seq, seq, seq, seq, seq, P(), P("fs", "tp"), P("tp"), P(),
            P("fs", "tp"), P("tp"), P("fs", "tp"), P("tp"), P("fs", "tp"), P("tp"),
        ),
        out_specs=seq,
        check_vma=False,
    )
```

```python
import functools

import jax
import jax.numpy as jnp
from jax import lax
from jax.experimental import pallas as pl
from jax.experimental.pallas import tpu as pltpu
from jax.sharding import PartitionSpec as P

MESH = pl.DeviceIdType.MESH
F32, BF16 = jnp.float32, jnp.bfloat16
EPS = 1e-06

RELAY_Z = [(0, 1, 0), (0, -1, 0), (1, 2, 0), (-1, -2, 0), (2, 3, 0), (-2, -3, 0), (3, 4, 1), (-3, -4, 2)]
DIRECT_Z = [(0, 1, 0), (0, -1, 0), (0, 2, 0), (0, -2, 0), (0, 3, 0), (0, -3, 0), (0, 4, 1), (0, -4, 2)]
SKIP_Z = [(0, 1, 0), (0, -1, 0), (0, 2, 0), (0, -2, 0), (2, 3, 0), (-2, -3, 0), (2, 4, 1), (-2, -4, 2)]
RELAY_Y = [(0, 1, 0), (0, -1, 0), (1, 2, 1), (-1, -2, 2)]
DIRECT_Y = [(0, 1, 0), (0, -1, 0), (0, 2, 1), (0, -2, 2)]
OFFSETS = (0, 1, -1, 2, -2, 3, -3, 4)

STAGES = ((32, SKIP_Z, DIRECT_Y), (16, RELAY_Z, RELAY_Y), (32, RELAY_Z, RELAY_Y))
HALVES = 2
N_GATHER = 52
N_REDUCE = 7 * HALVES
N_SPREAD = 7 * HALVES
N_COPIES = 3 * N_GATHER + 2 * N_REDUCE + N_SPREAD

ORDER = (
    ("A0", "B0", "C0", "pre", "att0", "att1", "att2", "att3", "A1", "B1", "A2", "B2", "C1", "A9"),
    ("B3", "R0", "R1", "C2", "R2", "B4", "C3", "S0", "B5", "C4", "S1", "B6", "C5", "S2", "C6", "B9"),
    ("H0", "C9", "D0", "D1", "D2", "O0"),
)


def dot_rows(a, b):
    return lax.dot_general(a, b, (((1,), (1,)), ((), ())), preferred_element_type=F32)


def dot_plain(a, b):
    return lax.dot_general(a, b, (((1,), (0,)), ((), ())), preferred_element_type=F32)


def kernel(*refs):
    inputs, rest = refs[:16], refs[16:]
    upd_ref, tot_ref = rest[:2]
    staged, rest = rest[2:18], rest[18:]
    (
        wa, wb, wc, lc, mc, nrm, hid, uall, nin,
        px, pr, own, sa, sb, sc, ra, rb, rc,
        load_sem, send_sem, recv_sem,
    ) = rest
    res, q, k, v, lod, sur, hg, ow, ocs, png, gw, gcs, uw, ucs, dw, dcs = staged
    rep, fs, tp = (lax.axis_index(n) for n in ("rep", "fs", "tp"))
    zl, y = lax.div(fs, 4), lax.rem(fs, 4)
    x, c = lax.div(tp, 2), lax.rem(tp, 2)
    z = rep * 8 + zl
    sgn = 1 - 2 * c

    def at(dz=0, dy=0):
        zz = lax.rem(z + dz + 32, 32)
        return (lax.div(zz, 8), lax.rem(zz, 8) * 4 + lax.rem(y + dy + 4, 4), tp)

    def at_x(dx):
        return (rep, fs, 2 * lax.rem(x + dx + 4, 4) + c)

    partner = (rep, fs, 2 * x + 1 - c)

    class Copy:
        def __init__(self, i):
            self.i, self.sent, self.got = i, None, False

        def start(self, src, dst, to):
            self.sent = pltpu.make_async_remote_copy(
                src_ref=src, dst_ref=dst, send_sem=send_sem.at[self.i], recv_sem=recv_sem.at[self.i],
                device_id=to, device_id_type=MESH)
            self.sent.start()

        def wait(self, dst, to):
            if not self.got:
                self.got = True
                pltpu.make_async_remote_copy(
                    src_ref=dst, dst_ref=dst, send_sem=send_sem.at[self.i], recv_sem=recv_sem.at[self.i],
                    device_id=to, device_id_type=MESH).wait_recv()

    copies = [Copy(i) for i in range(N_COPIES)]
    free = iter(copies)

    barrier = pltpu.get_barrier_semaphore()
    peers = []
    dzs = sorted({child - parent for _, tree, _ in STAGES for parent, child, _ in tree})
    dys = sorted({child - parent for _, _, tree in STAGES for parent, child, _ in tree} - {-2})
    peers += [at(dz=d) for d in dzs] + [at(dy=d) for d in dys] + [at_x(1), at_x(-1), partner]
    for peer in peers:
        pl.semaphore_signal(barrier, inc=1, device_id=peer, device_id_type=MESH)

    loads = [pltpu.make_async_copy(inputs[i], staged[i], load_sem.at[i]) for i in range(16)]
    for i in (7, 10, 12, 14, 4, 5, 1, 2, 3, 6, 0, 8, 9, 11, 13, 15):
        loads[i].start()
    for i in (7, 10, 12, 14):
        loads[i].wait()
    wa[zl, y] = ow[...].astype(BF16)
    zpad = jnp.zeros((64, 32), BF16)
    wb[zl, y, :, 0:352] = gw[...].astype(BF16)
    wb[zl, y, :, 352:384] = zpad
    wb[zl, y, :, 384:736] = uw[...].astype(BF16)
    wb[zl, y, :, 736:768] = zpad
    wc[zl, y, :, 0:352] = dw[...].astype(BF16)
    wc[zl, y, :, 352:384] = zpad
    pl.semaphore_wait(barrier, len(peers))

    def stage_steps(buf, p, ztree, ytree):
        cp = {}

        def plane(d):
            return lax.rem(zl - d + 8, 8)

        def q_ref(dz, dy, zpart, ypart):
            rows = 64 - p
            cut = 16 * (rows // 32) if rows > 16 else 0
            lo, hi = p, 64
            for part in (zpart, ypart):
                if part == 1:
                    hi = p + cut
                if part == 2:
                    lo = p + cut
            return buf.at[plane(dz), lax.rem(y - dy + 4, 4), lo:hi]

        def p_ref(dy, part):
            lo, hi = (0, p)
            if p > 16:
                if part == 1:
                    hi = p // 2
                if part == 2:
                    lo = p // 2
            return buf.at[zl, lax.rem(y - dy + 4, 4), lo:hi]

        def b_ref(dz, part):
            lo, hi = (0, 4) if part == 0 else ((0, 2) if part == 1 else (2, 4))
            return buf.at[plane(dz), lo:hi, 0:p]

        def p_skip(part):
            return p <= 16 and part == 2

        table = {}
        for parent, child, part in ytree:
            if p and not p_skip(part):
                table["py", child] = (parent, part)
        for parent, child, part in ztree:
            if p:
                table["pz", child] = (parent, part)
            table["qz", child] = (parent, part)
        for d in OFFSETS:
            for parent, child, part in ytree:
                table["qy", d, child] = (parent, part)
        for key in table:
            cp[key] = next(free)

        def refs(key, back):
            parent, part = table[key]
            d = parent if back else key[-1]
            step = key[-1] - parent
            if key[0] == "py":
                return p_ref(d, part), at(dy=step)
            if key[0] == "pz":
                return b_ref(d, part), at(dz=step)
            if key[0] == "qz":
                return q_ref(d, 0, part, 0), at(dz=step)
            return q_ref(key[1], d, 0, part), at(dy=step)

        def send(key):
            if key not in table:
                return
            parent = table[key][0]
            if key[0] in ("py", "qz"):
                if parent:
                    wait(key[:-1] + (parent,))
            elif key[0] == "pz":
                if parent:
                    wait(("pz", parent))
                else:
                    for n in (1, -1, 2, -2):
                        wait(("py", n))
            else:
                if parent:
                    wait(key[:-1] + (parent,))
                elif key[1] == 4:
                    wait(("qz", 4))
                    wait(("qz", -4))
                elif key[1]:
                    wait(("qz", key[1]))
            src, to = refs(key, True)
            cp[key].start(src, src, to)

        def wait(key):
            if key in table:
                dst, to = refs(key, False)
                cp[key].wait(dst, to)

        depth = {0: 0}
        for parent, child, _ in ztree:
            depth[child] = depth[parent] + 1
        last = max(depth.values())
        steps = []

        def add(r, key):
            while len(steps) <= r:
                steps.append([])
            steps[r].append(key)

        for key in [("py", 1), ("py", -1)]:
            add(0, key)
        ydepth = {0: 0}
        for parent, child, _ in ytree:
            ydepth[child] = ydepth[parent] + 1
        for key in [("py", 2), ("py", -2)]:
            add(ydepth[2] - 1, key)
        for parent, child, _ in ztree:
            add(depth[child] - 1, ("qz", child))
            add(depth[child] - 1 + ydepth[2], ("pz", child))
        for d in OFFSETS:
            for child in (1, -1):
                add(depth[d], ("qy", d, child))
            for child in (2, -2):
                add(depth[d] + ydepth[2] - 1, ("qy", d, child))

        def run(r):
            if r < len(steps):
                for key in steps[r]:
                    send(key)
            if r == 9:
                for key in table:
                    wait(key)

        return run

    stage = {
        "A": stage_steps(wa, *STAGES[0]),
        "B": stage_steps(wb, *STAGES[1]),
        "C": stage_steps(wc, *STAGES[2]),
    }

    def pre():
        for i in (4, 5, 1, 2, 3, 6, 0, 8, 9, 11, 13, 15):
            loads[i].wait()
        u = lod[...]
        ls = -(jnp.maximum(-u, 0.0) + jnp.log1p(jnp.exp(-jnp.abs(u)))) * (1.0 / 16.0)
        row = lax.broadcasted_iota(jnp.int32, (256, 256), 0)
        col = lax.broadcasted_iota(jnp.int32, (256, 256), 1)
        tri = jnp.where(col <= row, 1.0, 0.0).astype(BF16)
        hi = ls.astype(BF16)
        r1 = ls - hi.astype(F32)
        mid = r1.astype(BF16)
        lo = (r1 - mid.astype(F32)).astype(BF16)
        total = dot_plain(tri, hi) + (dot_plain(tri, mid) + dot_plain(tri, lo))
        srow = jnp.broadcast_to(sur[...], (256, 256))
        upto = jnp.sum(jnp.where(col <= row, srow, 0.0), axis=1, keepdims=True)
        before = jnp.sum(jnp.where(col < row, srow, 0.0), axis=1, keepdims=True)
        lc[...] = total + upto
        mc[...] = (total - ls) + before

    def attend(i):
        a, b = 64 * i, 64 * i + 64
        li, mi = lc[a:b], mc[a:b]
        qi, ki = q[a:b].astype(F32), k[a:b].astype(F32)
        mid = lc[a + 31 : a + 32]
        sf = dot_rows((qi * jnp.exp(li - mid)).astype(BF16), (ki * jnp.exp(mid - li)).astype(BF16))
        sb_ = dot_rows((qi * jnp.exp(mid - mi)).astype(BF16), (ki * jnp.exp(mi - mid)).astype(BF16))
        row = lax.broadcasted_iota(jnp.int32, (64, 64), 0)
        col = lax.broadcasted_iota(jnp.int32, (64, 64), 1)
        s = jnp.where(col <= row, sf, 0.0) + jnp.where(col >= row, sb_, 0.0)
        o = dot_plain(s.astype(BF16), v[a:b])
        if i > 0:
            edge = lc[a - 1 : a]
            kf = (k[0:a].astype(F32) * jnp.exp(edge - lc[0:a])).astype(BF16)
            s = dot_rows((qi * jnp.exp(li - edge)).astype(BF16), kf)
            o += dot_plain(s.astype(BF16), v[0:a])
        if i < 3:
            edge = lc[b - 1 : b]
            kb = (k[b:256].astype(F32) * jnp.exp(mc[b:256] - edge)).astype(BF16)
            s = dot_rows((qi * jnp.exp(edge - mi)).astype(BF16), kb)
            o += dot_plain(s.astype(BF16), v[b:256])
        o = o * (1.0 / 16.0)
        ms = jnp.mean(o * o, axis=1, keepdims=True)
        nrm[a:b] = (o * lax.rsqrt(ms + EPS) * hg[...]).astype(BF16)

    def ring_x(r, s):
        return lax.rem(x + (2, 4 - s, 4 + s, 0)[r], 4)

    T = 256 // HALVES

    def reducer(idx, lhs, weights):
        cps = [[next(free) for _ in range(7)] for _ in range(HALVES)]

        def w(j):
            full = weights[j]
            return full.reshape(256, full.shape[-1])

        def rows(h):
            return slice(h * T, h * T + T)

        def across(h, r):
            px[idx, h, r] = dot_rows(lhs[rows(h)], w(2 * ring_x(r, -sgn) + 1 - c)).astype(BF16)
            cps[h][r].start(px.at[idx, h, r], pr.at[idx, h, r], partner)

        def mine(h, r):
            own[h, r] = dot_rows(lhs[rows(h)], w(2 * ring_x(r, sgn) + c))

        def pair(h, r):
            cps[h][r].wait(pr.at[idx, h, r], partner)
            return own[h, r] + pr[idx, h, r].astype(F32)

        def first():
            for h in range(HALVES):
                across(h, 0)
            for h in range(HALVES):
                mine(h, 0)
                across(h, 1)
            for h in range(HALVES):
                sa[idx, h] = pair(h, 0).astype(BF16)
                cps[h][4].start(sa.at[idx, h], ra.at[idx, h], at_x(sgn))
                across(h, 2)

        def second():
            for h in range(HALVES):
                mine(h, 1)
                sb[idx, h] = pair(h, 1).astype(BF16)
                cps[h][5].start(sb.at[idx, h], rb.at[idx, h], at_x(-sgn))
            for h in range(HALVES):
                mine(h, 2)
                across(h, 3)
            for h in range(HALVES):
                own[h, 2] = pair(h, 2)

        def third():
            for h in range(HALVES):
                cps[h][4].wait(ra.at[idx, h], at_x(sgn))
                sc[idx, h] = (own[h, 2] + ra[idx, h].astype(F32)).astype(BF16)
                cps[h][6].start(sc.at[idx, h], rc.at[idx, h], at_x(sgn))
            for h in range(HALVES):
                mine(h, 3)
            for h in range(HALVES):
                own[h, 3] = pair(h, 3)

        def total(h):
            cp = cps[h]
            cp[5].wait(rb.at[idx, h], at_x(-sgn))
            cp[6].wait(rc.at[idx, h], at_x(sgn))
            return own[h, 3] + rb[idx, h].astype(F32) + rc[idx, h].astype(F32)

        return first, second, third, total, rows

    mix = reducer(0, nrm, wa)
    down = reducer(1, hid, wc)

    cps = [[next(free) for _ in range(7)] for _ in range(HALVES)]

    def u_ref(h, j):
        return uall.at[j, h * T : h * T + T]

    def spread_own(h):
        cp = cps[h]
        total = mix[3](h)
        sl = mix[4](h)
        u = (res[sl].astype(F32) + ocs[...] * total).astype(BF16)
        uall[tp, sl] = u
        upd_ref[sl] = u
        cp[0].start(u_ref(h, tp), u_ref(h, tp), at_x(sgn))
        cp[1].start(u_ref(h, tp), u_ref(h, tp), at_x(-sgn))
        cp[3].start(u_ref(h, tp), u_ref(h, tp), partner)

    def spread_on(h):
        cp = cps[h]
        j = 2 * ring_x(1, sgn) + c
        cp[0].wait(u_ref(h, j), at_x(sgn))
        cp[2].start(u_ref(h, j), u_ref(h, j), at_x(sgn))
        cp[4].start(u_ref(h, j), u_ref(h, j), partner)
        j = 2 * ring_x(2, sgn) + c
        cp[1].wait(u_ref(h, j), at_x(-sgn))
        cp[5].start(u_ref(h, j), u_ref(h, j), partner)

    def spread_end(h):
        cp = cps[h]
        j = 2 * ring_x(0, sgn) + c
        cp[2].wait(u_ref(h, j), at_x(sgn))
        cp[6].start(u_ref(h, j), u_ref(h, j), partner)

    def normalise(h):
        cp = cps[h]
        for n, r in ((3, 3), (4, 1), (5, 2), (6, 0)):
            cp[n].wait(u_ref(h, 2 * ring_x(r, -sgn) + 1 - c), partner)
        sl = mix[4](h)
        ssq = jnp.zeros((T, 1), F32)
        for j in range(8):
            u = uall[j, sl].astype(F32)
            ssq += jnp.sum(u * u, axis=1, keepdims=True)
        factor = lax.rsqrt(ssq * (1.0 / 2048.0) + EPS)
        for j in range(8):
            u = uall[j, sl].astype(F32)
            nin[sl, 256 * j : 256 * j + 256] = (u * factor * png[:, 256 * j : 256 * j + 256]).astype(BF16)

    def hidden(h):
        normalise(h)
        sl = mix[4](h)
        gu = dot_plain(nin[sl], wb[...].reshape(2048, 768))
        g = gu[:, 0:352] * gcs[...]
        up = gu[:, 384:736] * ucs[...]
        hid[sl, 0:352] = (g / (1.0 + jnp.exp(-g)) * up).astype(BF16)
        hid[sl, 352:384] = jnp.zeros((T, 32), BF16)

    def out(h):
        sl = mix[4](h)
        tot_ref[sl] = dcs[...] * down[3](h)

    whole = {"R0": mix[0], "R1": mix[1], "R2": mix[2], "D0": down[0], "D1": down[1], "D2": down[2]}
    per_half = {
        "S0": spread_own, "S1": spread_on, "S2": spread_end,
        "H0": hidden, "O0": out,
    }

    for token in sum(ORDER, ()):
        if token[0] in stage:
            stage[token[0]](int(token[1:]))
        elif token == "pre":
            pre()
        elif token[:3] == "att":
            attend(int(token[3:]))
        elif token in whole:
            whole[token]()
        elif token[2:] == "":
            for h in range(HALVES):
                per_half[token](h)
        else:
            per_half[token[:2]](int(token[2:]))

    for cp in copies:
        if cp.sent is not None:
            cp.sent.wait_send()


def body(res, q, k, v, lod, sur, hg, ow, ocs, png, gw, gcs, uw, ucs, dw, dcs):
    rows = 256
    flat = (
        res.reshape(rows, -1), q.reshape(rows, -1), k.reshape(rows, -1), v.reshape(rows, -1),
        lod.reshape(rows, -1), sur.reshape(1, rows), hg.reshape(1, -1), ow, ocs.reshape(1, -1),
        png.reshape(1, -1), gw, gcs, uw, ucs, dw, dcs.reshape(1, -1),
    )
    H, T = HALVES, 256 // HALVES
    vm = pltpu.VMEM
    upd, total = pl.pallas_call(
        kernel,
        name="layer",
        out_shape=(pltpu.VMEM((rows, 256), BF16), pltpu.VMEM((rows, 256), F32)),
        in_specs=[pl.BlockSpec(memory_space=pl.ANY)] * 16,
        out_specs=[pl.BlockSpec(memory_space=pltpu.VMEM)] * 2,
        scratch_shapes=[vm(a.shape, a.dtype) for a in flat] + [
            vm((8, 4, 64, 256), BF16), vm((8, 4, 64, 768), BF16), vm((8, 4, 64, 384), BF16),
            vm((256, 256), F32), vm((256, 256), F32), vm((256, 256), BF16), vm((256, 384), BF16),
            vm((8, 256, 256), BF16), vm((256, 2048), BF16),
            vm((2, H, 4, T, 256), BF16), vm((2, H, 4, T, 256), BF16), vm((H, 4, T, 256), F32),
            vm((2, H, T, 256), BF16), vm((2, H, T, 256), BF16), vm((2, H, T, 256), BF16),
            vm((2, H, T, 256), BF16), vm((2, H, T, 256), BF16), vm((2, H, T, 256), BF16),
            pltpu.SemaphoreType.DMA((16,)),
            pltpu.SemaphoreType.DMA((N_COPIES,)), pltpu.SemaphoreType.DMA((N_COPIES,)),
        ],
        compiler_params=pltpu.CompilerParams(
            collective_id=0, has_side_effects=True, vmem_limit_bytes=56 * 2**20),
    )(*flat)
    result = (upd.astype(F32) + total).astype(BF16)
    return result.reshape(1, rows, 256)


def solution(mesh):
    seq = P(("rep", "fs"), None, "tp")
    return jax.shard_map(
        body,
        mesh=mesh,
        in_specs=(
            seq, seq, seq, seq, seq, seq, P(), P("fs", "tp"), P("tp"), P(),
            P("fs", "tp"), P("tp"), P("fs", "tp"), P("tp"), P("fs", "tp"), P("tp"),
        ),
        out_specs=seq,
        check_vma=False,
    )
```
